512 devices in a mesh: kv: 128 (over z, x, core), tp: 4 (over y).
Axes of the slice: x: 4, y: 4, z: 16, core: 2. Of those that a mesh axis runs over, the one named last changes fastest.
Arguments:
- tokens: bfloat16 [4, 4096], P(None, 'kv'), may hold values from -30 to 30
- norm_gain: float32 [4096], P('kv'), may hold values from 0.1 to 1.9
- query_weight: bfloat16 [4096, 2048], P('kv', 'tp'), may hold values from -0.09375 to 0.09375
- cache_keys: bfloat16 [4, 65536, 16, 128], P(None, 'kv', 'tp'), may hold values from -180 to 180
- cache_values: bfloat16 [4, 65536, 16, 128], P(None, 'kv', 'tp'), may hold values from -6 to 6
- lengths: int32 [4], replicated, may hold values from 32769 to 65536, as said below
- lambdas: float32 [16], P('tp'), may hold values from 0.3 to 0.8
- head_gain: float32 [128], replicated, may hold values from 0.1 to 1.9
- out_weight: bfloat16 [2048, 4096], P('tp', 'kv'), may hold values from -0.125 to 0.125
Outputs:
- mixed: bfloat16 [4, 4096], P(None, 'kv')
The draws below stay inside these ranges and needn't reach their ends.
Inputs may be any that keep to these rules, and one draw needn't show every extreme that they name: `lengths`: every length is more than half of 65536; some sequence has exactly 65536.
All inputs are finite; a program needn't handle non-finite values.
Results may differ from the reference program's by a relative error of at most 0.02.
Values may be sent and summed in bfloat16 or wider, within the bound.
A program may use at most 64 MiB of HBM per device.

```python
import math
import jax
import jax.numpy as jnp
from jax import lax

D = 4096
HEADS = 16
HD = 64
VD = 128
SEQS = 4
LENGTH = 65536
N_TP = 4


def draw_tokens(key, part):
    first = jax.random.fold_in(jax.random.fold_in(key, 11), 0)
    second = jax.random.fold_in(jax.random.fold_in(key, 11), 1)
    fourth = jax.random.fold_in(jax.random.fold_in(key, 11), 3)
    column = jnp.arange(D, dtype=jnp.int32)
    phase = jax.random.uniform(first, (), jnp.float32, 0.0, 2.0 * math.pi)
    blocks = jnp.exp(jax.random.uniform(second, (D // 32,), jnp.float32, math.log(0.6), math.log(1.7)))
    scale = jnp.exp(1.2 * jnp.sin(2.0 * math.pi * column.astype(jnp.float32) / D + phase)) * blocks[column // 32]
    base = jnp.clip(jax.random.normal(fourth, (SEQS, D), jnp.float32), -4.5, 4.5)
    return (base * scale[None, :]).astype(jnp.bfloat16)


def draw_cache_keys(key, part):
    key_drawn = jax.random.fold_in(jax.random.fold_in(key, 23), 4)
    shape = (SEQS, LENGTH, HEADS, 2 * HD)
    base = jnp.clip(1.75 * jax.random.normal(key_drawn, shape, jnp.float32), -7.0, 7.0)
    return base.astype(jnp.bfloat16)


def draw_lengths(key, part):
    first, second = jax.random.split(jax.random.fold_in(key, 37))
    value_rows = jax.random.randint(first, (SEQS,), LENGTH // 2 + 1, LENGTH + 1)
    chosen = jax.random.randint(second, (), 0, SEQS)
    return jnp.where(jnp.arange(SEQS, dtype=jnp.int32) == chosen, LENGTH, value_rows).astype(jnp.int32)


def block_levels(rng, shape, cuts, low, top_value):
    level, own = 1.0, jax.random.fold_in(rng, 6)
    for position, parts in cuts:
        heights = jnp.exp(jax.random.uniform(jax.random.fold_in(own, position), (parts,), jnp.float32, low / len(cuts), top_value / len(cuts)))
        level = level * jnp.repeat(heights, shape[position] // parts).reshape([-1 if axis == position else 1 for axis in range(len(shape))])
    return level


def scatter_about(key, shape, width, limit, cuts=(), held_as=jnp.bfloat16):
    array = width * jax.random.normal(key, shape, jnp.float32)
    if cuts:
        array = array * block_levels(key, shape, cuts, -0.22, 0.18)
    return jnp.clip(array, -limit, limit).astype(held_as)


def setup_inputs(seed: int = 0) -> dict:
    splits = jax.random.split(jax.random.key(seed), 10)
    tokens = draw_tokens(jax.random.fold_in(splits[9], 71), 0)
    norm_gain = jnp.clip(1.0 + 0.18 * jax.random.normal(splits[1], (D,), jnp.float32), 0.1, 1.9)
    query_weight = scatter_about(splits[2], (D, HEADS * 2 * HD), D ** -0.5, 0.09375, ((0, 128), (1, 4)))
    cache_keys = draw_cache_keys(jax.random.fold_in(splits[9], 71), 0)
    cache_values = scatter_about(splits[4], (SEQS, LENGTH, HEADS, VD), 1.0, 6.0, ((1, 128), (2, 4)))
    lengths = draw_lengths(jax.random.fold_in(splits[9], 71), 0)
    lambdas = jnp.clip(0.3 + 0.5 * jax.random.uniform(splits[6], (HEADS,), jnp.float32) ** block_levels(splits[6], (HEADS,), ((0, 4),), -0.2, 0.2), 0.3, 0.8)
    head_gain = jnp.clip(1.0 + 0.18 * jax.random.normal(splits[7], (VD,), jnp.float32), 0.1, 1.9)
    out_weight = scatter_about(splits[8], (HEADS * VD, D), (HEADS * VD) ** -0.5, 0.125, ((0, 4), (1, 128)))
    return {"tokens": tokens, "norm_gain": norm_gain, "query_weight": query_weight, "cache_keys": cache_keys, "cache_values": cache_values, "lengths": lengths, "lambdas": lambdas, "head_gain": head_gain, "out_weight": out_weight}


eps = 1e-06
NEG = -1e+30

def reference(tokens, norm_gain, query_weight, cache_keys, cache_values, lengths, lambdas, head_gain, out_weight):
    floats = tokens.astype(jnp.float32)
    squares = lax.optimization_barrier(jnp.sum(floats * floats, axis=1))
    scaled_logits = (floats * norm_gain).astype(jnp.bfloat16)
    projected = jnp.dot(scaled_logits, query_weight, preferred_element_type=jnp.float32)
    inverse = lax.rsqrt(squares / D + eps)
    query = (projected * inverse[:, None] * 0.125).astype(jnp.bfloat16).reshape(SEQS, HEADS, 2, HD)
    keys = cache_keys.reshape(SEQS, LENGTH, HEADS, 2, HD)

    def one_sequence(args):
        query_row, key_rows_block, vrows, length = args
        score_matrix = jnp.einsum('yvn,wyvn->yvw', query_row.astype(jnp.float32), key_rows_block.astype(jnp.float32))
        valid = (jnp.arange(LENGTH, dtype=jnp.int32) < length)[None, None, :]
        score_matrix = jnp.where(valid, score_matrix, NEG)
        peak = lax.optimization_barrier(jnp.max(score_matrix, axis=-1, keepdims=True))
        weights = jnp.where(valid, jnp.exp(score_matrix - peak), 0.0)
        mass = lax.optimization_barrier(jnp.sum(weights, axis=-1))
        rounded = lax.optimization_barrier(weights.astype(jnp.bfloat16)).astype(jnp.float32)
        summed = jnp.einsum('hmp,phv->hmv', rounded, vrows.astype(jnp.float32))
        return summed / mass[..., None]
    ratios = lax.map(one_sequence, (query, keys, cache_values, lengths))
    attended = ratios[:, :, 0] - lambdas[None, :, None] * ratios[:, :, 1]
    normed = attended * lax.rsqrt(lax.optimization_barrier(jnp.mean(attended * attended, axis=-1, keepdims=True)) + eps) * head_gain * 0.8
    normed = normed.astype(jnp.bfloat16).reshape(SEQS, HEADS * VD)
    rows = HEADS * VD // N_TP
    total = jnp.zeros((SEQS, D), jnp.float32)
    for group in range(N_TP):
        part = jnp.dot(normed[:, group * rows:(group + 1) * rows], out_weight[group * rows:(group + 1) * rows], preferred_element_type=jnp.float32).astype(jnp.bfloat16)
        total = total + part.astype(jnp.float32)
    return total.astype(jnp.bfloat16)
```

```python
import functools

import jax
import jax.numpy as jnp
from jax import lax
from jax.experimental import pallas as pl
from jax.experimental.pallas import tpu as pltpu
from jax.sharding import PartitionSpec as P

MESH = pl.DeviceIdType.MESH
D = 4096
HD = 64
NEAR = 8
FAR = 16
GROUPS = 4
SEQS = 4
HEADS = 4
eps = 1e-06
NEG = -1e30
F32 = jnp.float32
BF16 = jnp.bfloat16


def kernel(
    tokens_hbm, gain_hbm, wq_hbm, keys_hbm, values_hbm, lengths_hbm, lambdas_hbm, hgain_hbm, wo_hbm,
    out_ref,
    tokens, gain, wq, keys, values, lengths, lambdas, hgain, wo,
    a_send, a_near, a_far, qbuf, c_send, c_near, c_far, nbuf, pbuf,
    small_sem, kv_sem, send_sem, a_near_sem, a_far_sem, q_sem, c_near_sem, c_far_sem, n_sem, p_sem,
):
    kv = lax.axis_index("kv")
    tp = lax.axis_index("tp")
    near = lax.rem(kv, NEAR)
    far = kv // NEAR
    core = lax.rem(near, 2)
    chip = near // 2
    span = keys.shape[1] // HEADS

    def near_id(d):
        return (far * NEAR + lax.rem(near + d, NEAR), tp)

    def far_id(d):
        return (lax.rem(far + d, FAR) * NEAR + near, tp)

    def group_id(d):
        return (kv, lax.rem(tp + d, GROUPS))

    barrier = pltpu.get_barrier_semaphore()
    for d in range(1, FAR):
        pl.semaphore_signal(barrier, inc=1, device_id=far_id(d), device_id_type=MESH)
    for d in range(1, NEAR):
        pl.semaphore_signal(barrier, inc=1, device_id=near_id(d), device_id_type=MESH)
    for d in range(1, GROUPS):
        pl.semaphore_signal(barrier, inc=1, device_id=group_id(d), device_id_type=MESH)

    small = [
        pltpu.make_async_copy(src, dst, small_sem.at[k])
        for k, (src, dst) in enumerate(
            [
                (tokens_hbm, tokens), (gain_hbm, gain), (wq_hbm, wq), (lengths_hbm, lengths),
                (lambdas_hbm, lambdas), (hgain_hbm, hgain), (wo_hbm, wo),
            ]
        )
    ]
    for copy in small:
        copy.start()
    cache = []
    for s in range(SEQS):
        cache.append(pltpu.make_async_copy(keys_hbm.at[s], keys.at[s], kv_sem.at[s]))
        cache.append(pltpu.make_async_copy(values_hbm.at[s], values.at[s], kv_sem.at[SEQS + s]))
    for copy in cache:
        copy.start()
    for copy in small[:3]:
        copy.wait()

    floats = tokens[...].astype(F32)
    squares = jnp.sum(floats * floats, axis=1, keepdims=True)
    scaled = (floats * gain[...]).astype(BF16)
    partial = jnp.dot(scaled, wq[...], preferred_element_type=F32)
    for s in range(SEQS):
        for half in range(2):
            for r in range(2):
                c = (2 * half + r) * 128
                a_send[2 * s + half, r : r + 1, :] = partial[s : s + 1, c : c + 128]
            a_send[2 * s + half, 2:3, :] = jnp.broadcast_to(squares[s : s + 1, :], (1, 128))

    pl.semaphore_wait(barrier, FAR + NEAR + GROUPS - 3)

    sends = []

    def send(src, dst, recv, device):
        copy = pltpu.make_async_remote_copy(
            src_ref=src, dst_ref=dst, send_sem=send_sem.at[len(sends)], recv_sem=recv,
            device_id=device, device_id_type=MESH,
        )
        copy.start()
        sends.append(copy)

    def landed(buf, slot, sem):
        pltpu.make_async_copy(buf.at[slot], buf.at[slot], sem.at[slot]).wait()

    for d in range(1, NEAR):
        j = lax.rem(near + d, NEAR)
        send(a_send.at[j], a_near.at[near], a_near_sem.at[near], near_id(d))
    a_near[near] = a_send[near]
    for d in range(1, NEAR):
        landed(a_near, lax.rem(near + d, NEAR), a_near_sem)
    a_far[far] = jnp.sum(a_near[...], axis=0)
    for d in (8, 7, 9, 6, 10, 5, 11, 4, 12, 3, 13, 2, 14, 1, 15):
        send(a_far.at[far], a_far.at[far], a_far_sem.at[far], far_id(d))
    for d in range(1, FAR):
        landed(a_far, lax.rem(far + d, FAR), a_far_sem)
    total = jnp.sum(a_far[...], axis=0)
    inverse = lax.rsqrt(total[2:3, :] / D + eps)
    qbuf[near] = (total[0:2, :] * inverse * 0.125).astype(BF16).astype(F32)
    for d in (4, 5, 3, 2, 6, 7, 1):
        send(qbuf.at[near], qbuf.at[near], q_sem.at[near], near_id(d))
    for copy in small[3:]:
        copy.wait()

    width = keys.shape[1]
    row = lax.broadcasted_iota(jnp.int32, (2 * HEADS, width), 0)
    column = lax.broadcasted_iota(jnp.int32, (2 * HEADS, width), 1)
    own_head = (column % HEADS) == (row // 2)
    lane8 = lax.broadcasted_iota(jnp.int32, (2 * HEADS, 128), 1)
    row8 = lax.broadcasted_iota(jnp.int32, (2 * HEADS, 128), 0)
    map_lanes = (lane8 // HD) == (row8 % 2)

    for turn in (0, 1, 3, 2):
        s = lax.rem(chip + turn, SEQS)
        for half in range(2):
            if turn:
                landed(qbuf, 2 * s + half, q_sem)
        if not turn:
            landed(qbuf, 2 * s + 1 - core, q_sem)
        heads = []
        for h in range(HEADS):
            line = qbuf[2 * s + h // 2, h % 2 : h % 2 + 1, :]
            heads += [line, line]
        q8 = jnp.where(map_lanes, jnp.concatenate(heads, axis=0), 0.0).astype(BF16)
        pltpu.make_async_copy(keys_hbm.at[s], keys.at[s], kv_sem.at[s]).wait()
        scores = lax.dot_general(
            q8, keys[s], (((1,), (1,)), ((), ())), preferred_element_type=F32
        )
        valid = own_head & (column < (lengths[s] - kv * span) * HEADS)
        scores = jnp.where(valid, scores, NEG)
        peak = jnp.max(scores, axis=1, keepdims=True)
        weights = jnp.where(valid, jnp.exp(scores - peak), 0.0)
        mass = jnp.sum(weights, axis=1, keepdims=True)
        pltpu.make_async_copy(values_hbm.at[s], values.at[s], kv_sem.at[SEQS + s]).wait()
        summed = jnp.dot(weights.astype(BF16), values[s], preferred_element_type=F32)
        stats = jnp.sum(
            jnp.where(lane8 == row8, mass, 0.0) + jnp.where(lane8 == row8 + 8, peak, 0.0),
            axis=0, keepdims=True,
        )
        for half in range(2):
            c_send[2 * s + half, 0:4, :] = summed[4 * half : 4 * half + 4, :]
            c_send[2 * s + half, 4:5, :] = stats
        if turn:
            for half in range(2):
                send(
                    c_send.at[2 * s + half], c_near.at[near], c_near_sem.at[near],
                    (far * NEAR + 2 * s + half, tp),
                )
        else:
            send(
                c_send.at[2 * s + 1 - core], c_near.at[near], c_near_sem.at[near],
                (far * NEAR + 2 * s + 1 - core, tp),
            )
            c_near[near] = c_send[near]

    def merged(box, first):
        count = box.shape[0]
        lane = lax.broadcasted_iota(jnp.int32, (count, 4, 128), 2)
        line = lax.broadcasted_iota(jnp.int32, (count, 4, 128), 1)
        both = box[:, 4:5, :]
        masses = jnp.sum(jnp.where(lane == line + first, both, 0.0), axis=2, keepdims=True)
        peaks = jnp.sum(jnp.where(lane == line + first + 8, both, 0.0), axis=2, keepdims=True)
        top = jnp.max(peaks, axis=0, keepdims=True)
        factor = jnp.exp(peaks - top)
        return top[0], jnp.sum(masses * factor, axis=0), jnp.sum(box[:, 0:4, :] * factor, axis=0)

    for d in range(1, NEAR):
        landed(c_near, lax.rem(near + d, NEAR), c_near_sem)
    peak, mass, summed = merged(c_near[...], 4 * core)
    lane4 = lax.broadcasted_iota(jnp.int32, (4, 128), 1)
    row4 = lax.broadcasted_iota(jnp.int32, (4, 128), 0)
    stats = jnp.sum(
        jnp.where(lane4 == row4, mass, 0.0) + jnp.where(lane4 == row4 + 8, peak, 0.0),
        axis=0, keepdims=True,
    )
    c_far[far, 0:4, :] = summed
    c_far[far, 4:5, :] = stats
    for d in (8, 7, 9, 6, 10, 5, 11, 4, 12, 3, 13, 2, 14, 1, 15):
        send(c_far.at[far], c_far.at[far], c_far_sem.at[far], far_id(d))
    for d in range(1, FAR):
        landed(c_far, lax.rem(far + d, FAR), c_far_sem)
    peak, mass, summed = merged(c_far[...], 0)
    ratio = summed / mass
    lines = []
    for h in range(2):
        attended = ratio[2 * h : 2 * h + 1, :] - lambdas[2 * core + h] * ratio[2 * h + 1 : 2 * h + 2, :]
        mean = jnp.mean(attended * attended, axis=1, keepdims=True)
        lines.append(attended * lax.rsqrt(mean + eps) * hgain[...] * 0.8)
    nbuf[near] = jnp.concatenate(lines, axis=0).astype(BF16).astype(F32)
    for d in (4, 5, 3, 2, 6, 7, 1):
        send(nbuf.at[near], nbuf.at[near], n_sem.at[near], near_id(d))
    for d in range(1, NEAR):
        landed(nbuf, lax.rem(near + d, NEAR), n_sem)
    part = jnp.zeros((SEQS, 32), F32)
    for h in range(HEADS):
        head = jnp.concatenate(
            [nbuf[2 * s + h // 2, h % 2 : h % 2 + 1, :] for s in range(SEQS)], axis=0
        ).astype(BF16)
        part += lax.dot_general(
            head, wo[:, 128 * h : 128 * (h + 1)], (((1,), (1,)), ((), ())),
            preferred_element_type=F32,
        )
    part = part.astype(BF16).astype(F32)
    pbuf[tp] = jnp.concatenate([part, jnp.zeros((SEQS, 96), F32)], axis=1)
    for d in (2, 1, 3):
        send(pbuf.at[tp], pbuf.at[tp], p_sem.at[tp], group_id(d))
    for d in range(1, GROUPS):
        landed(pbuf, lax.rem(tp + d, GROUPS), p_sem)
    out_ref[...] = jnp.sum(pbuf[...], axis=0)[:, 0:32].astype(BF16)
    for copy in sends:
        copy.wait_send()


def body(tokens, norm_gain, query_weight, cache_keys, cache_values, lengths, lambdas, head_gain, out_weight):
    seqs, span, heads, size = cache_keys.shape
    hbm = pl.BlockSpec(memory_space=pltpu.HBM)
    n_sends = 7 + 15 + 7 + 7 + 15 + 7 + 3
    return pl.pallas_call(
        kernel,
        name="decode",
        out_shape=jax.ShapeDtypeStruct((seqs, 32), BF16),
        in_specs=[hbm] * 9,
        out_specs=pl.BlockSpec(memory_space=pltpu.VMEM),
        scratch_shapes=[
            pltpu.VMEM((seqs, 32), BF16),
            pltpu.VMEM((1, 32), F32),
            pltpu.VMEM((32, 512), BF16),
            pltpu.VMEM((seqs, span * heads, size), BF16),
            pltpu.VMEM((seqs, span * heads, size), BF16),
            pltpu.SMEM((seqs,), jnp.int32),
            pltpu.SMEM((heads,), F32),
            pltpu.VMEM((1, 128), F32),
            pltpu.VMEM((32, 512), BF16),
            pltpu.VMEM((NEAR, 3, 128), F32),
            pltpu.VMEM((NEAR, 3, 128), F32),
            pltpu.VMEM((FAR, 3, 128), F32),
            pltpu.VMEM((NEAR, 2, 128), F32),
            pltpu.VMEM((NEAR, 5, 128), F32),
            pltpu.VMEM((NEAR, 5, 128), F32),
            pltpu.VMEM((FAR, 5, 128), F32),
            pltpu.VMEM((NEAR, 2, 128), F32),
            pltpu.VMEM((GROUPS, SEQS, 128), F32),
            pltpu.SemaphoreType.DMA((7,)),
            pltpu.SemaphoreType.DMA((2 * SEQS,)),
            pltpu.SemaphoreType.DMA((n_sends,)),
            pltpu.SemaphoreType.DMA((NEAR,)),
            pltpu.SemaphoreType.DMA((FAR,)),
            pltpu.SemaphoreType.DMA((NEAR,)),
            pltpu.SemaphoreType.DMA((NEAR,)),
            pltpu.SemaphoreType.DMA((FAR,)),
            pltpu.SemaphoreType.DMA((NEAR,)),
            pltpu.SemaphoreType.DMA((GROUPS,)),
        ],
        compiler_params=pltpu.CompilerParams(
            collective_id=0, has_side_effects=True
        ),
    )(
        tokens,
        norm_gain.reshape(1, 32),
        query_weight,
        cache_keys.reshape(seqs, span * heads, size),
        cache_values.reshape(seqs, span * heads, size),
        lengths,
        lambdas,
        head_gain.reshape(1, 128),
        out_weight.T,
    )


def solution(mesh):
    in_specs = (
        P(None, "kv"), P("kv"), P("kv", "tp"), P(None, "kv", "tp", None), P(None, "kv", "tp", None),
        P(), P("tp"), P(), P("tp", "kv"),
    )
    return jax.shard_map(body, mesh=mesh, in_specs=in_specs, out_specs=P(None, "kv"), check_vma=False)
```

```python
import functools

import jax
import jax.numpy as jnp
from jax import lax
from jax.experimental import pallas as pl
from jax.experimental.pallas import tpu as pltpu
from jax.sharding import PartitionSpec as P

MESH = pl.DeviceIdType.MESH
D = 4096
HD = 64
NEAR = 8
FAR = 16
GROUPS = 4
SEQS = 4
HEADS = 4
eps = 1e-06
NEG = -1e30
F32 = jnp.float32
BF16 = jnp.bfloat16


def kernel(
    tokens_hbm, gain_hbm, wq_hbm, keys_hbm, values_hbm, lengths_hbm, lambdas_hbm, hgain_hbm, wo_hbm,
    out_ref,
    tokens, gain, wq, keys, values, lengths, lambdas, hgain, wo,
    a_send, a_near, a_far, qbuf, c_send, c_near, c_far, nbuf, pbuf,
    small_sem, kv_sem, send_sem, recv_sem, q_sem, known_sem,
):
    kv = lax.axis_index("kv")
    tp = lax.axis_index("tp")
    near = lax.rem(kv, NEAR)
    far = kv // NEAR
    core = lax.rem(near, 2)
    chip = near // 2
    span = keys.shape[1] // HEADS

    def near_id(d):
        return (far * NEAR + lax.rem(near + d, NEAR), tp)

    def far_id(d):
        return (lax.rem(far + d, FAR) * NEAR + near, tp)

    def group_id(d):
        return (kv, lax.rem(tp + d, GROUPS))

    barrier = pltpu.get_barrier_semaphore()
    for d in (2, 14, 1, 15):
        pl.semaphore_signal(barrier, inc=1, device_id=far_id(d), device_id_type=MESH)
    for d in (4, 5, 3, 2, 6, 7, 1):
        pl.semaphore_signal(barrier, inc=1, device_id=near_id(d), device_id_type=MESH)
    for d in (2, 1, 3):
        pl.semaphore_signal(barrier, inc=1, device_id=group_id(d), device_id_type=MESH)

    small = [
        pltpu.make_async_copy(src, dst, small_sem.at[k])
        for k, (src, dst) in enumerate(
            [
                (tokens_hbm, tokens), (gain_hbm, gain), (wq_hbm, wq), (lengths_hbm, lengths),
                (lambdas_hbm, lambdas), (hgain_hbm, hgain), (wo_hbm, wo),
            ]
        )
    ]
    for copy in small:
        copy.start()
    cache = []
    for s in range(SEQS):
        cache.append(pltpu.make_async_copy(keys_hbm.at[s], keys.at[s], kv_sem.at[s]))
        cache.append(pltpu.make_async_copy(values_hbm.at[s], values.at[s], kv_sem.at[SEQS + s]))
    for copy in cache:
        copy.start()
    for copy in small[:3]:
        copy.wait()

    floats = tokens[...].astype(F32)
    squares = jnp.sum(floats * floats, axis=1, keepdims=True)
    scaled = (floats * gain[...]).astype(BF16)
    partial = jnp.dot(scaled, wq[...], preferred_element_type=F32)
    for s in range(SEQS):
        for half in range(2):
            for r in range(2):
                c = (2 * half + r) * 128
                a_send[2 * s + half, r : r + 1, :] = partial[s : s + 1, c : c + 128]
            a_send[2 * s + half, 2:3, :] = jnp.broadcast_to(squares[s : s + 1, :], (1, 128))

    pl.semaphore_wait(barrier, 4 + NEAR - 1 + GROUPS - 1)

    def send(phase, src, dst, recv, device):
        pltpu.make_async_remote_copy(
            src_ref=src, dst_ref=dst, send_sem=send_sem.at[phase], recv_sem=recv,
            device_id=device, device_id_type=MESH,
        ).start()

    def arrived(buf, count, sem):
        view = buf.at[pl.ds(0, count)]
        pltpu.make_async_copy(view, view, sem).wait()

    for d in (4, 5, 3, 2, 6, 7, 1):
        j = lax.rem(near + d, NEAR)
        send(0, a_send.at[j], a_near.at[near], recv_sem.at[0], near_id(d))
    for d, sem in ((2, known_sem.at[0]), (4, known_sem.at[1])):
        for e in (d, FAR - d):
            pl.semaphore_signal(sem, inc=1, device_id=far_id(e), device_id_type=MESH)
        if d == 2:
            pl.semaphore_wait(sem, 2)
    a_near[near] = a_send[near]
    arrived(a_near, NEAR - 1, recv_sem.at[0])
    a_far[far] = jnp.sum(a_near[...], axis=0)
    pl.semaphore_wait(known_sem.at[1], 2)
    for d in (8, 7, 9, 6, 10, 5, 11, 4, 12, 3, 13, 2, 14, 1, 15):
        send(1, a_far.at[far], a_far.at[far], recv_sem.at[1], far_id(d))
    arrived(a_far, FAR - 1, recv_sem.at[1])
    total = jnp.sum(a_far[...], axis=0)
    inverse = lax.rsqrt(total[2:3, :] / D + eps)
    qbuf[near] = (total[0:2, :] * inverse * 0.125).astype(BF16).astype(F32)
    for d in (4, 5, 3, 2, 6, 7, 1):
        send(2, qbuf.at[near], qbuf.at[near], q_sem.at[chip], near_id(d))
    for copy in small[3:]:
        copy.wait()

    width = keys.shape[1]
    row = lax.broadcasted_iota(jnp.int32, (2 * HEADS, width), 0)
    column = lax.broadcasted_iota(jnp.int32, (2 * HEADS, width), 1)
    own_head = (column % HEADS) == (row // 2)
    lane8 = lax.broadcasted_iota(jnp.int32, (2 * HEADS, 128), 1)
    row8 = lax.broadcasted_iota(jnp.int32, (2 * HEADS, 128), 0)
    map_lanes = (lane8 // HD) == (row8 % 2)

    for turn in (0, 1, 3, 2):
        s = lax.rem(chip + turn, SEQS)
        arrived(qbuf, 2 if turn else 1, q_sem.at[s])
        heads = []
        for h in range(HEADS):
            line = qbuf[2 * s + h // 2, h % 2 : h % 2 + 1, :]
            heads += [line, line]
        q8 = jnp.where(map_lanes, jnp.concatenate(heads, axis=0), 0.0).astype(BF16)
        pltpu.make_async_copy(keys_hbm.at[s], keys.at[s], kv_sem.at[s]).wait()
        scores = lax.dot_general(
            q8, keys[s], (((1,), (1,)), ((), ())), preferred_element_type=F32
        )
        valid = own_head & (column < (lengths[s] - kv * span) * HEADS)
        scores = jnp.where(valid, scores, NEG)
        peak = jnp.max(scores, axis=1, keepdims=True)
        weights = jnp.where(valid, jnp.exp(scores - peak), 0.0)
        mass = jnp.sum(weights, axis=1, keepdims=True)
        pltpu.make_async_copy(values_hbm.at[s], values.at[s], kv_sem.at[SEQS + s]).wait()
        summed = jnp.dot(weights.astype(BF16), values[s], preferred_element_type=F32)
        stats = jnp.sum(
            jnp.where(lane8 == row8, mass, 0.0) + jnp.where(lane8 == row8 + 8, peak, 0.0),
            axis=0, keepdims=True,
        )
        for half in range(2):
            c_send[2 * s + half, 0:4, :] = summed[4 * half : 4 * half + 4, :]
            c_send[2 * s + half, 4:5, :] = stats
        if turn:
            for half in range(2):
                send(
                    3, c_send.at[2 * s + half], c_near.at[near], recv_sem.at[2],
                    (far * NEAR + 2 * s + half, tp),
                )
        else:
            send(
                3, c_send.at[2 * s + 1 - core], c_near.at[near], recv_sem.at[2],
                (far * NEAR + 2 * s + 1 - core, tp),
            )
            c_near[near] = c_send[near]

    def merged(box, first):
        count = box.shape[0]
        lane = lax.broadcasted_iota(jnp.int32, (count, 4, 128), 2)
        line = lax.broadcasted_iota(jnp.int32, (count, 4, 128), 1)
        both = box[:, 4:5, :]
        masses = jnp.sum(jnp.where(lane == line + first, both, 0.0), axis=2, keepdims=True)
        peaks = jnp.sum(jnp.where(lane == line + first + 8, both, 0.0), axis=2, keepdims=True)
        top = jnp.max(peaks, axis=0, keepdims=True)
        factor = jnp.exp(peaks - top)
        return top[0], jnp.sum(masses * factor, axis=0), jnp.sum(box[:, 0:4, :] * factor, axis=0)

    arrived(c_near, NEAR - 1, recv_sem.at[2])
    peak, mass, summed = merged(c_near[...], 4 * core)
    lane4 = lax.broadcasted_iota(jnp.int32, (4, 128), 1)
    row4 = lax.broadcasted_iota(jnp.int32, (4, 128), 0)
    stats = jnp.sum(
        jnp.where(lane4 == row4, mass, 0.0) + jnp.where(lane4 == row4 + 8, peak, 0.0),
        axis=0, keepdims=True,
    )
    c_far[far, 0:4, :] = summed
    c_far[far, 4:5, :] = stats
    for d in (8, 7, 9, 6, 10, 5, 11, 4, 12, 3, 13, 2, 14, 1, 15):
        send(4, c_far.at[far], c_far.at[far], recv_sem.at[3], far_id(d))
    arrived(c_far, FAR - 1, recv_sem.at[3])
    peak, mass, summed = merged(c_far[...], 0)
    ratio = summed / mass
    lines = []
    for h in range(2):
        attended = ratio[2 * h : 2 * h + 1, :] - lambdas[2 * core + h] * ratio[2 * h + 1 : 2 * h + 2, :]
        mean = jnp.mean(attended * attended, axis=1, keepdims=True)
        lines.append(attended * lax.rsqrt(mean + eps) * hgain[...] * 0.8)
    nbuf[near] = jnp.concatenate(lines, axis=0).astype(BF16).astype(F32)
    for d in (4, 5, 3, 2, 6, 7, 1):
        send(5, nbuf.at[near], nbuf.at[near], recv_sem.at[4], near_id(d))
    arrived(nbuf, NEAR - 1, recv_sem.at[4])
    part = jnp.zeros((SEQS, 32), F32)
    for h in range(HEADS):
        head = jnp.concatenate(
            [nbuf[2 * s + h // 2, h % 2 : h % 2 + 1, :] for s in range(SEQS)], axis=0
        ).astype(BF16)
        part += lax.dot_general(
            head, wo[:, 128 * h : 128 * (h + 1)], (((1,), (1,)), ((), ())),
            preferred_element_type=F32,
        )
    part = part.astype(BF16).astype(F32)
    pbuf[tp] = jnp.concatenate([part, jnp.zeros((SEQS, 96), F32)], axis=1)
    for d in (2, 1, 3):
        send(6, pbuf.at[tp], pbuf.at[tp], recv_sem.at[5], group_id(d))
    for phase, (buf, count) in enumerate(
        ((a_send, NEAR), (a_far, FAR), (qbuf, NEAR), (c_send, NEAR), (c_far, FAR), (nbuf, NEAR), (pbuf, GROUPS))
    ):
        arrived(buf, count - 1, send_sem.at[phase])
    arrived(pbuf, GROUPS - 1, recv_sem.at[5])
    out_ref[...] = jnp.sum(pbuf[...], axis=0)[:, 0:32].astype(BF16)


def body(tokens, norm_gain, query_weight, cache_keys, cache_values, lengths, lambdas, head_gain, out_weight):
    seqs, span, heads, size = cache_keys.shape
    hbm = pl.BlockSpec(memory_space=pltpu.HBM)
    return pl.pallas_call(
        kernel,
        name="decode",
        out_shape=jax.ShapeDtypeStruct((seqs, 32), BF16),
        in_specs=[hbm] * 9,
        out_specs=pl.BlockSpec(memory_space=pltpu.VMEM),
        scratch_shapes=[
            pltpu.VMEM((seqs, 32), BF16),
            pltpu.VMEM((1, 32), F32),
            pltpu.VMEM((32, 512), BF16),
            pltpu.VMEM((seqs, span * heads, size), BF16),
            pltpu.VMEM((seqs, span * heads, size), BF16),
            pltpu.SMEM((seqs,), jnp.int32),
            pltpu.SMEM((heads,), F32),
            pltpu.VMEM((1, 128), F32),
            pltpu.VMEM((32, 512), BF16),
            pltpu.VMEM((NEAR, 3, 128), F32),
            pltpu.VMEM((NEAR, 3, 128), F32),
            pltpu.VMEM((FAR, 3, 128), F32),
            pltpu.VMEM((NEAR, 2, 128), F32),
            pltpu.VMEM((NEAR, 5, 128), F32),
            pltpu.VMEM((NEAR, 5, 128), F32),
            pltpu.VMEM((FAR, 5, 128), F32),
            pltpu.VMEM((NEAR, 2, 128), F32),
            pltpu.VMEM((GROUPS, SEQS, 128), F32),
            pltpu.SemaphoreType.DMA((7,)),
            pltpu.SemaphoreType.DMA((2 * SEQS,)),
            pltpu.SemaphoreType.DMA((7,)),
            pltpu.SemaphoreType.DMA((6,)),
            pltpu.SemaphoreType.DMA((SEQS,)),
            pltpu.SemaphoreType.REGULAR((2,)),
        ],
        compiler_params=pltpu.CompilerParams(
            collective_id=0, has_side_effects=True
        ),
    )(
        tokens,
        norm_gain.reshape(1, 32),
        query_weight,
        cache_keys.reshape(seqs, span * heads, size),
        cache_values.reshape(seqs, span * heads, size),
        lengths,
        lambdas,
        head_gain.reshape(1, 128),
        out_weight.T,
    )


def solution(mesh):
    in_specs = (
        P(None, "kv"), P("kv"), P("kv", "tp"), P(None, "kv", "tp", None), P(None, "kv", "tp", None),
        P(), P("tp"), P(), P("tp", "kv"),
    )
    return jax.shard_map(body, mesh=mesh, in_specs=in_specs, out_specs=P(None, "kv"), check_vma=False)
```
